32 devices in a mesh: fs: 8 (over z, y), tp: 4 (over x, core).
Axes of the slice: x: 2, y: 2, z: 4, core: 2. Of those that a mesh axis runs over, the one named last changes fastest.
Arguments:
- saved_input: bfloat16 [65536, 2048], P(('fs', 'tp')), may hold values from -500 to 500
- value_cotangent: bfloat16 [65536, 1024], P(('fs', 'tp')), may hold values from -500 to 500
- hidden_input: bfloat16 [65536, 1024], P(('fs', 'tp')), may hold values from -500 to 500
- out_cotangent: bfloat16 [65536, 2048], P(('fs', 'tp')), may hold values from -500 to 500
- value_factor: bfloat16 [2048, 256], P('fs'), may hold values from -2 to 2
- out_factor: bfloat16 [1024, 256], P('fs'), may hold values from -2 to 2
- value_weight: float32 [2048, 1024], P('fs', 'tp'), may hold values from -0.125 to 0.125
- out_weight: float32 [1024, 2048], P('fs', 'tp'), may hold values from -0.1875 to 0.1875
- value_first: float32 [256, 1024], P('fs', 'tp'), may hold values from -1.2 to 1.2
- value_second: float32 [256, 1024], P('fs', 'tp'), may hold values from 0.02 to 0.5
- out_first: float32 [256, 2048], P('fs', 'tp'), may hold values from -1.2 to 1.2
- out_second: float32 [256, 2048], P('fs', 'tp'), may hold values from 0.02 to 0.5
Outputs:
- value_update: float32 [2048, 1024], P('fs', 'tp')
- out_update: float32 [1024, 2048], P('fs', 'tp')
- new_value_weight: float32 [2048, 1024], P('fs', 'tp')
- new_out_weight: float32 [1024, 2048], P('fs', 'tp')
- value_copy: bfloat16 [2048, 1024], P(None, 'tp')
- out_copy: bfloat16 [1024, 2048], P(None, 'tp')
- new_value_first: float32 [256, 1024], P('fs', 'tp')
- new_value_second: float32 [256, 1024], P('fs', 'tp')
- new_out_first: float32 [256, 2048], P('fs', 'tp')
- new_out_second: float32 [256, 2048], P('fs', 'tp')
The draws below stay inside these ranges and needn't reach their ends.
All inputs are finite; a program needn't handle non-finite values.
Results may differ from the reference program's by a relative error of at most 0.0065.
Values may be sent and summed in bfloat16 or wider, within the bound.
A program may use at most 128 MiB of HBM per device.

```python
import math
import jax
import jax.numpy as jnp
from jax import lax

D = 2048
DM = 1024
R = 256
TOKENS = 65536


def scaled_field(key, rows, cols, base, row_spread):
    keys = jax.random.split(key, 3)
    field = jnp.clip(jax.random.normal(keys[0], (rows, cols), jnp.float32), -4.0, 4.0)
    row_level = row_spread * jax.random.uniform(keys[1], (rows, 1), jnp.float32)
    column_level = 0.5 * jnp.arange(cols, dtype=jnp.float32)[None, :] / cols
    column_level = column_level + 0.5 * jax.random.uniform(keys[2], (1, cols), jnp.float32)
    return base * field * jnp.power(10.0, row_level + column_level)


def draw_saved_input(key, part):
    return scaled_field(jax.random.fold_in(key, 11), TOKENS, D, 1.0, 1.0).astype(jnp.bfloat16)


def draw_value_cotangent(key, part):
    return scaled_field(jax.random.fold_in(key, 12), TOKENS, DM, 1.0, 1.0).astype(jnp.bfloat16)


def draw_hidden_input(key, part):
    return scaled_field(jax.random.fold_in(key, 13), TOKENS, DM, 1.0, 1.0).astype(jnp.bfloat16)


def draw_out_cotangent(key, part):
    return scaled_field(jax.random.fold_in(key, 14), TOKENS, D, 1.0, 1.0).astype(jnp.bfloat16)


def draw_value_factor(key, part):
    return scaled_field(jax.random.fold_in(key, 15), D, R, 0.04, 0.0).astype(jnp.bfloat16)


def draw_out_factor(key, part):
    return scaled_field(jax.random.fold_in(key, 16), DM, R, 0.04, 0.0).astype(jnp.bfloat16)


def steps_of(key, shape, shards, low, high):
    def one(dim, parts):
        steps = jax.random.uniform(jax.random.fold_in(jax.random.fold_in(key, 6), dim), (parts,), jnp.float32, low / len(shards), high / len(shards))
        return jnp.repeat(jnp.exp(steps), shape[dim] // parts).reshape((-1,) + (1,) * (len(shape) - dim - 1))

    factor_of = one(*shards[0])
    for cut in shards[1:]:
        factor_of = factor_of * one(*cut)
    return factor_of


def centred(key, dims, spread, limit, pieces=(), kind=jnp.bfloat16):
    values = spread * jax.random.normal(key, dims, jnp.float32)
    if pieces:
        values = values * steps_of(key, dims, pieces, -0.22, 0.18)
    return jnp.clip(values, -limit, limit).astype(kind)


def setup_inputs(seed: int = 0) -> dict:
    seeds = jax.random.split(jax.random.key(seed), 13)
    return {
        "saved_input": draw_saved_input(jax.random.fold_in(seeds[12], 71), 0),
        "value_cotangent": draw_value_cotangent(jax.random.fold_in(seeds[12], 71), 0),
        "hidden_input": draw_hidden_input(jax.random.fold_in(seeds[12], 71), 0),
        "out_cotangent": draw_out_cotangent(jax.random.fold_in(seeds[12], 71), 0),
        "value_factor": draw_value_factor(jax.random.fold_in(seeds[12], 71), 0),
        "out_factor": draw_out_factor(jax.random.fold_in(seeds[12], 71), 0),
        "value_weight": centred(seeds[6], (D, DM), D ** -0.5, 0.125, ((0, 8), (1, 4)), jnp.float32),
        "out_weight": centred(seeds[7], (DM, D), DM ** -0.5, 0.1875, ((0, 8), (1, 4)), jnp.float32),
        "value_first": centred(seeds[8], (R, DM), 0.2, 1.2, ((0, 8), (1, 4)), jnp.float32),
        "value_second": jnp.clip(jnp.exp(math.log(0.5) - 3.218876 * jax.random.uniform(seeds[9], (R, DM), jnp.float32) ** steps_of(seeds[9], (R, DM), ((0, 8), (1, 4)), -0.2, 0.2)), 0.02, 0.5),
        "out_first": centred(seeds[10], (R, D), 0.2, 1.2, ((0, 8), (1, 4)), jnp.float32),
        "out_second": jnp.clip(jnp.exp(math.log(0.5) - 3.218876 * jax.random.uniform(seeds[11], (R, D), jnp.float32) ** steps_of(seeds[11], (R, D), ((0, 8), (1, 4)), -0.2, 0.2)), 0.02, 0.5),
    }


momentum_decay = 0.9
square_decay = 0.95
adam_epsilon = 1e-08
update_scale = 0.25
learning_rate = 0.01

def moment_ratio(first, second, lowrank, clip_factor):
    scaled = clip_factor * lowrank
    new_first = momentum_decay * first + (1.0 - momentum_decay) * scaled
    new_second = square_decay * second + (1.0 - square_decay) * scaled * scaled
    ratio = new_first / (jnp.sqrt(new_second) + adam_epsilon)
    return (new_first, new_second, ratio)

def reference(saved_input, value_cotangent, hidden_input, out_cotangent, value_factor, out_factor, value_weight, out_weight, value_first, value_second, out_first, out_second):
    highest = lax.Precision.HIGHEST
    gradient_value = jnp.dot(saved_input.T, value_cotangent, preferred_element_type=jnp.float32)
    gradient_out = jnp.dot(hidden_input.T, out_cotangent, preferred_element_type=jnp.float32)
    value_basis = value_factor.astype(jnp.float32)
    out_basis = out_factor.astype(jnp.float32)
    low_value = jnp.dot(value_basis.T, gradient_value, precision=highest)
    low_out = jnp.dot(out_basis.T, gradient_out, precision=highest)
    total = jnp.sum(low_value * low_value) + jnp.sum(low_out * low_out)
    root_mean = jnp.sqrt(total / (R * (D + DM)))
    clip_factor = 1.0 / jnp.maximum(root_mean, 1.0)
    new_value_first, new_value_second, value_ratio = moment_ratio(value_first, value_second, low_value, clip_factor)
    new_out_first, new_out_second, out_ratio = moment_ratio(out_first, out_second, low_out, clip_factor)
    value_update = update_scale * jnp.dot(value_basis, value_ratio, precision=highest)
    out_update = update_scale * jnp.dot(out_basis, out_ratio, precision=highest)
    new_value_weight = value_weight - learning_rate * value_update
    new_out_weight = out_weight - learning_rate * out_update
    value_copy = new_value_weight.astype(jnp.bfloat16)
    out_copy = new_out_weight.astype(jnp.bfloat16)
    return (value_update, out_update, new_value_weight, new_out_weight, value_copy, out_copy, new_value_first, new_value_second, new_out_first, new_out_second)
```

```python
import functools

import jax
import jax.numpy as jnp
from jax import lax
from jax.experimental import pallas as pl
from jax.experimental.pallas import tpu as pltpu
from jax.sharding import PartitionSpec as P

momentum_decay = 0.9
square_decay = 0.95
adam_epsilon = 1e-08
update_scale = 0.25
learning_rate = 0.01

MESH = pl.DeviceIdType.MESH
CORES = 2
LANES = 128
f32 = jnp.float32
bf16 = jnp.bfloat16


def digits(fs, tp):
    xs = tp // CORES
    ys = xs if fs % xs == 0 else 1
    return fs // ys, ys, xs


def exchange_kernel(
    fs, tp,
    x_v, c_v, x_o, c_o, fac_v, fac_o, w_v, w_o, m1_v, m2_v, m1_o, m2_o,
    F, W_v, W_o, R, n1_v, n2_v, n1_o, n2_o,
    xv, cv, xo, co, hi, rest,
    wown_v, wown_o,
    cs_v, cr_v, cs_o, cr_o, keep_v, keep_o,
    xs_v, xr_v, xs_o, xr_o, acc_v, acc_o,
    ys_v, yr_v, ys_o, yr_o, mid_v, mid_o,
    zs_v, zr_v, zs_o, zr_o, sq_s, sq_r,
    load_sem, fa_s, fa_r, fb_s, fb_r, fc_s, fc_r,
    wl_sem, wz_s, wz_r, wy_s, wy_r,
    rc_s, rc_r, rx_s, rx_r, ry_s, ry_r, rz_s, rz_r, sq_ss, sq_rs, ra_s, ra_r,
):
    Z, Y, X = digits(fs, tp)
    n = fs * tp
    f = lax.axis_index("fs")
    t = lax.axis_index("tp")
    z, y = f // Y, f % Y
    x, c = t // CORES, t % CORES
    me = f * tp + t

    def remote(src, dst, ss, rs, fd, td):
        return pltpu.make_async_remote_copy(
            src_ref=src, dst_ref=dst, send_sem=ss, recv_sem=rs,
            device_id={"fs": fd, "tp": td}, device_id_type=MESH)

    loads = [
        pltpu.make_async_copy(a, b, load_sem.at[i])
        for i, (a, b) in enumerate(((x_o, xo), (c_o, co), (x_v, xv), (c_v, cv)))
    ]
    for cp in loads:
        cp.start()

    barrier = pltpu.get_barrier_semaphore()

    @pl.loop(1, n)
    def _(d):
        peer = lax.rem(me + d, n)
        pl.semaphore_signal(
            barrier, inc=1, device_id={"fs": peer // tp, "tp": lax.rem(peer, tp)},
            device_id_type=MESH)

    rv, ro = fac_v.shape[0], fac_o.shape[0]
    F[pl.ds(f, 1), :rv, :] = fac_v[...][None]
    F[pl.ds(f, 1), rv:, :] = fac_o[...][None]
    wown_v[...] = w_v[...].astype(bf16)
    wown_o[...] = w_o[...].astype(bf16)
    pl.semaphore_wait(barrier, n - 1)

    rx = (rv + ro) // X

    def piece(fi, xi, ci):
        return F.at[fi, pl.ds(pl.multiple_of(xi * rx, 16), rx),
                    pl.ds(pl.multiple_of(ci * LANES, LANES), LANES)]

    def half(fi, ci):
        return F.at[fi, :, pl.ds(pl.multiple_of(ci * LANES, LANES), LANES)]

    def fa(d, fi):
        return remote(piece(fi, x, c), piece(fi, x, c), fa_s.at[d - 1], fa_r.at[d - 1],
                      lax.rem(f + d, fs), t)

    for d in range(1, fs):
        fa(d, f).start()

    parts = ((0, wown_v, W_v), (1, wown_o, W_o))
    own_copies = [pltpu.make_async_copy(own, W.at[z, y], wl_sem.at[p]) for p, own, W in parts]
    for cp in own_copies:
        cp.start()

    def wz(p, W, s, up, zb, src=None):
        k = 0 if up else 1
        zd = z + 1 if up else z - 1
        return remote(W.at[zb, y] if src is None else src, W.at[zb, y],
                      wz_s.at[p, k, s], wz_r.at[p, k, s], zd * Y + y, t)

    def wy(p, W, zb, d, yb, src=None):
        return remote(W.at[zb, yb] if src is None else src, W.at[zb, yb],
                      wy_s.at[p, zb, d - 1], wy_r.at[p, zb, d - 1],
                      z * Y + lax.rem(y + d, Y), t)

    def weights_send(s):
        @pl.when((z >= s) & (z < Z - 1))
        def _():
            for p, own, W in parts:
                wz(p, W, s, True, z - s, own if s == 0 else None).start()

        @pl.when((z + s < Z) & (z > 0))
        def _():
            for p, own, W in parts:
                wz(p, W, s, False, z + s, own if s == 0 else None).start()

    def weights_receive(s):
        for up in (True, False):
            zb = z - 1 - s if up else z + 1 + s

            @pl.when((zb >= 0) if up else (zb < Z))
            def _():
                for p, own, W in parts:
                    wz(p, W, s, up, zb).wait_recv()
                    for d in range(1, Y):
                        wy(p, W, zb, d, y).start()

    weights_send(0)
    for p, own, W in parts:
        for d in range(1, Y):
            wy(p, W, z, d, y, own).start()

    def fb(d, k, fi, xi):
        return remote(piece(fi, xi, c), piece(fi, xi, c), fb_s.at[d - 1, k - 1],
                      fb_r.at[d - 1, k - 1], f, lax.rem(x + k, X) * CORES + c)

    def fc(d, fi, ci):
        return remote(half(fi, ci), half(fi, ci), fc_s.at[d - 1], fc_r.at[d - 1],
                      f, x * CORES + 1 - c)

    source = [lax.rem(f + fs - d, fs) for d in range(fs)]
    for d in range(1, fs):
        fa(d, source[d]).wait_recv()
        for k in range(1, X):
            fb(d, k, source[d], x).start()
    for d in range(1, fs):
        for k in range(1, X):
            fb(d, k, source[d], lax.rem(x + X - k, X)).wait_recv()
        fc(d, source[d], c).start()
    for d in range(1, fs):
        fc(d, source[d], 1 - c).wait_recv()

    tokens = xo.shape[0]
    step = tokens // 4

    def basis(x_ref, rows):
        @pl.loop(0, tokens // step)
        def _(i):
            at = pl.ds(pl.multiple_of(i * step, step), step)
            fac = F[:, rows, :].reshape(-1, F.shape[2])
            b = jnp.dot(x_ref[at, :], fac, preferred_element_type=f32).T
            high = b.astype(bf16)
            hi[:, at] = high
            rest[:, at] = (b - high.astype(f32)).astype(bf16)

    def product(c_ref, start, width):
        cols = c_ref[:, pl.ds(pl.multiple_of(start, LANES), width)]
        return (jnp.dot(hi[...], cols, preferred_element_type=f32)
                + jnp.dot(rest[...], cols, preferred_element_type=f32))

    def rc(p, send, recv, i):
        return remote(send.at[i], recv.at[i], rc_s.at[p, i], rc_r.at[p, i],
                      f, x * CORES + 1 - c)

    def multiply(p, c_ref, send, recv, keep):
        cb = keep.shape[2]

        @pl.loop(0, X)
        def _(i):
            send[i] = product(c_ref, (i * CORES + 1 - c) * cb, cb)
            rc(p, send, recv, i).start()

        @pl.loop(0, X)
        def _(i):
            keep[i] = product(c_ref, (i * CORES + c) * cb, cb)

    def sx(p, send, recv, k):
        xd = lax.rem(x + k, X)
        return remote(send.at[k - 1], recv.at[k - 1], rx_s.at[p, k - 1], rx_r.at[p, k - 1],
                      f, xd * CORES + c)

    def sy(p, send, recv, k):
        yd = lax.rem(y + k, Y)
        return remote(send.at[k - 1], recv.at[k - 1], ry_s.at[p, k - 1], ry_r.at[p, k - 1],
                      z * Y + yd, t)

    def sz(p, send, recv, k):
        zd = lax.rem(z + k, Z)
        return remote(send.at[k - 1], recv.at[k - 1], rz_s.at[p, k - 1], rz_r.at[p, k - 1],
                      zd * Y + y, t)

    def to_x(p, cs, cr, keep, send, recv):
        for i in range(X):
            rc(p, cs, cr, i).wait_recv()
        for k in range(1, X):
            xd = lax.rem(x + k, X)
            send[k - 1] = (keep[xd] + cr[xd]).astype(bf16)
            sx(p, send, recv, k).start()

    def to_y(p, cr, keep, xsend, recv, acc, send, yrecv):
        total = keep[x] + cr[x]
        for k in range(1, X):
            sx(p, xsend, recv, k).wait_recv()
            total = total + recv[k - 1].astype(f32)
        acc[...] = total.reshape(acc.shape)
        for k in range(1, Y):
            yd = lax.rem(y + k, Y)
            send[k - 1] = acc[:, pl.ds(yd, 1)][:, 0].astype(bf16)
            sy(p, send, yrecv, k).start()

    def to_z(p, acc, ysend, recv, mid, send, zrecv):
        total = acc[:, pl.ds(y, 1)][:, 0]
        for k in range(1, Y):
            sy(p, ysend, recv, k).wait_recv()
            total = total + recv[k - 1].astype(f32)
        mid[...] = total
        for k in range(1, Z):
            send[k - 1] = mid[lax.rem(z + k, Z)].astype(bf16)
            sz(p, send, zrecv, k).start()

    def finish(p, mid, send, recv):
        total = mid[z]
        for k in range(1, Z):
            sz(p, send, recv, k).wait_recv()
            total = total + recv[k - 1].astype(f32)
        return total

    loads[0].wait()
    basis(xo, slice(rv, rv + ro))
    loads[1].wait()
    multiply(1, co, cs_o, cr_o, keep_o)
    to_x(1, cs_o, cr_o, keep_o, xs_o, xr_o)
    if Z > 1:
        weights_receive(0)
    if Z > 2:
        weights_send(1)
    loads[2].wait()
    basis(xv, slice(0, rv))
    loads[3].wait()
    multiply(0, cv, cs_v, cr_v, keep_v)
    to_x(0, cs_v, cr_v, keep_v, xs_v, xr_v)
    to_y(1, cr_o, keep_o, xs_o, xr_o, acc_o, ys_o, yr_o)
    to_y(0, cr_v, keep_v, xs_v, xr_v, acc_v, ys_v, yr_v)
    to_z(1, acc_o, ys_o, yr_o, mid_o, zs_o, zr_o)
    to_z(0, acc_v, ys_v, yr_v, mid_v, zs_v, zr_v)
    for s in range(1, Z - 1):
        weights_receive(s)
        if s + 1 < Z - 1:
            weights_send(s + 1)
    low_o = finish(1, mid_o, zs_o, zr_o)
    low_v = finish(0, mid_v, zs_v, zr_v)

    square = jnp.sum(low_o * low_o) + jnp.sum(low_v * low_v)
    sq_s[...] = jnp.full(sq_s.shape, square, f32)

    @pl.loop(1, n)
    def _(d):
        peer = lax.rem(me + d, n)
        remote(sq_s, sq_r.at[d - 1], sq_ss.at[d - 1], sq_rs.at[d - 1],
               peer // tp, lax.rem(peer, tp)).start()

    @pl.loop(1, n)
    def _(d):
        remote(sq_s, sq_r.at[d - 1], sq_ss.at[d - 1], sq_rs.at[d - 1], f, t).wait_recv()

    total = jnp.sum(sq_r[...], axis=0)[0:1, 0:1] + square
    count = hi.shape[0] * (cv.shape[1] + co.shape[1])
    clip = 1.0 / jnp.maximum(jnp.sqrt(total / count), 1.0)

    def moments(low, m1, m2, n1, n2):
        scaled = clip * low
        first = momentum_decay * m1[...] + (1.0 - momentum_decay) * scaled
        second = square_decay * m2[...] + (1.0 - square_decay) * scaled * scaled
        n1[...] = first
        n2[...] = second
        return (first / (jnp.sqrt(second) + adam_epsilon)).astype(bf16)

    cbv = low_v.shape[1]
    R[pl.ds(f, 1), :, :cbv] = moments(low_v, m1_v, m2_v, n1_v, n2_v)[None]
    R[pl.ds(f, 1), :, cbv:] = moments(low_o, m1_o, m2_o, n1_o, n2_o)[None]

    def ra(d, fi):
        return remote(R.at[fi], R.at[fi], ra_s.at[d - 1], ra_r.at[d - 1], lax.rem(f + d, fs), t)

    for d in range(1, fs):
        ra(d, f).start()

    for cp in own_copies:
        cp.wait()
    for s in range(Z - 1):
        @pl.when((z >= s) & (z < Z - 1))
        def _():
            for p, own, W in parts:
                wz(p, W, s, True, z - s, own if s == 0 else None).wait_send()

        @pl.when((z + s < Z) & (z > 0))
        def _():
            for p, own, W in parts:
                wz(p, W, s, False, z + s, own if s == 0 else None).wait_send()
    for p, own, W in parts:
        for zb in range(Z):
            for d in range(1, Y):
                wy(p, W, zb, d, y).wait_send()
                wy(p, W, zb, d, lax.rem(y + Y - d, Y)).wait_recv()
    for d in range(1, fs):
        fa(d, f).wait_send()
        for k in range(1, X):
            fb(d, k, source[d], x).wait_send()
        fc(d, source[d], c).wait_send()
    for p, cs, cr, xsnd, xrcv, ysnd, yrcv, zsnd, zrcv in (
        (0, cs_v, cr_v, xs_v, xr_v, ys_v, yr_v, zs_v, zr_v),
        (1, cs_o, cr_o, xs_o, xr_o, ys_o, yr_o, zs_o, zr_o),
    ):
        for i in range(X):
            rc(p, cs, cr, i).wait_send()
        for k in range(1, X):
            sx(p, xsnd, xrcv, k).wait_send()
        for k in range(1, Y):
            sy(p, ysnd, yrcv, k).wait_send()
        for k in range(1, Z):
            sz(p, zsnd, zrcv, k).wait_send()

    @pl.loop(1, n)
    def _(d):
        remote(sq_s, sq_r.at[d - 1], sq_ss.at[d - 1], sq_rs.at[d - 1], f, t).wait_send()

    for d in range(1, fs):
        ra(d, f).wait_send()
        ra(d, source[d]).wait_recv()


def update_kernel(fs, F, R, W_v, W_o, w_v, w_o, u_v, u_o, nw_v, nw_o, copy_v, copy_o):
    f = lax.axis_index("fs")
    rv, ro = w_v.shape[0], w_o.shape[0]
    cbv = w_v.shape[1]
    rank = F.shape[2]
    ratio = R[...].reshape(rank, -1)
    rate = learning_rate * update_scale

    for rows, cols, W, w, u, nw, copy in (
        (slice(0, rv), slice(0, cbv), W_v, w_v, u_v, nw_v, copy_v),
        (slice(rv, rv + ro), slice(cbv, None), W_o, w_o, u_o, nw_o, copy_o),
    ):
        k = w.shape[0]
        fac = F[:, rows, :].reshape(fs * k, rank)
        all_rows = jnp.dot(fac, ratio[:, cols], preferred_element_type=f32)
        copy[...] = (W[...].astype(f32).reshape(all_rows.shape) - rate * all_rows).astype(bf16)
        mine = jnp.dot(F[pl.ds(f, 1), rows, :][0], ratio[:, cols], preferred_element_type=f32)
        update = update_scale * mine
        u[...] = update
        nw[...] = w[...] - learning_rate * update


def solution(mesh):
    fs, tp = mesh.shape["fs"], mesh.shape["tp"]
    Z, Y, X = digits(fs, tp)

    def shards(x_v, c_v, x_o, c_o, fac_v, fac_o, w_v, w_o, m1_v, m2_v, m1_o, m2_o):
        rank = fac_v.shape[1]
        rr = rank // fs
        cbv, cbo = w_v.shape[1], w_o.shape[1]
        tokens = x_v.shape[0]
        vmem = pl.BlockSpec(memory_space=pltpu.VMEM)
        hbm = pl.BlockSpec(memory_space=pl.ANY)
        sds = jax.ShapeDtypeStruct
        V = pltpu.VMEM
        dma = pltpu.SemaphoreType.DMA

        def both(shape_of, dtype, copies=2):
            out = []
            for cb in (cbv, cbo):
                out += [V(shape_of(cb), dtype)] * copies
            return out

        x1, y1, z1 = max(X - 1, 1), max(Y - 1, 1), max(Z - 1, 1)
        scratch = [
            V(x_v.shape, bf16), V(c_v.shape, bf16), V(x_o.shape, bf16), V(c_o.shape, bf16),
            V((rank, tokens), bf16), V((rank, tokens), bf16),
            V(w_v.shape, bf16), V(w_o.shape, bf16),
            *both(lambda cb: (X, rank, cb), f32), *both(lambda cb: (X, rank, cb), f32, 1),
            *both(lambda cb: (x1, rank, cb), bf16),
            *both(lambda cb: (Z, Y, rr, cb), f32, 1),
            *both(lambda cb: (y1, Z, rr, cb), bf16),
            *both(lambda cb: (Z, rr, cb), f32, 1),
            *both(lambda cb: (z1, rr, cb), bf16),
            V((1, LANES), f32), V((fs * tp - 1, 1, LANES), f32),
            dma((4,)), dma((fs - 1,)), dma((fs - 1,)), dma((fs - 1, x1)), dma((fs - 1, x1)),
            dma((fs - 1,)), dma((fs - 1,)),
            dma((2,)), dma((2, 2, z1)), dma((2, 2, z1)), dma((2, Z, y1)), dma((2, Z, y1)),
            dma((2, X)), dma((2, X)), dma((2, x1)), dma((2, x1)), dma((2, y1)), dma((2, y1)),
            dma((2, z1)), dma((2, z1)), dma((fs * tp - 1,)), dma((fs * tp - 1,)),
            dma((fs - 1,)), dma((fs - 1,)),
        ]
        rows = fac_v.shape[0] + fac_o.shape[0]
        F, W_v, W_o, R, n1_v, n2_v, n1_o, n2_o = pl.pallas_call(
            functools.partial(exchange_kernel, fs, tp),
            out_shape=(
                sds((fs, rows, rank), bf16), sds((Z, Y) + w_v.shape, bf16),
                sds((Z, Y) + w_o.shape, bf16), sds((fs, rr, cbv + cbo), bf16),
                sds(m1_v.shape, f32), sds(m2_v.shape, f32),
                sds(m1_o.shape, f32), sds(m2_o.shape, f32),
            ),
            in_specs=[hbm] * 4 + [vmem] * 8,
            out_specs=(vmem, hbm, hbm, vmem, vmem, vmem, vmem, vmem),
            scratch_shapes=scratch,
            compiler_params=pltpu.CompilerParams(
                collective_id=0, has_side_effects=True, vmem_limit_bytes=60 * 1024 * 1024),
            name="exchange",
        )(x_v, c_v, x_o, c_o, fac_v, fac_o, w_v, w_o, m1_v, m2_v, m1_o, m2_o)
        outs = pl.pallas_call(
            functools.partial(update_kernel, fs),
            out_shape=(
                sds(w_v.shape, f32), sds(w_o.shape, f32),
                sds(w_v.shape, f32), sds(w_o.shape, f32),
                sds((fs * w_v.shape[0], cbv), bf16), sds((fs * w_o.shape[0], cbo), bf16),
            ),
            in_specs=[vmem] * 6,
            out_specs=(vmem,) * 6,
            compiler_params=pltpu.CompilerParams(vmem_limit_bytes=48 * 1024 * 1024),
            name="update",
        )(F, R, W_v, W_o, w_v, w_o)
        return (*outs, n1_v, n2_v, n1_o, n2_o)

    fsp = P(("fs", "tp"), None)
    both = P("fs", "tp")
    return jax.shard_map(
        shards,
        mesh=mesh,
        in_specs=(fsp,) * 4 + (P("fs", None),) * 2 + (both,) * 6,
        out_specs=(both,) * 4 + (P(None, "tp"),) * 2 + (both,) * 4,
        check_vma=False,
    )
```

```python
import functools

import jax
import jax.numpy as jnp
from jax import lax
from jax.experimental import pallas as pl
from jax.experimental.pallas import tpu as pltpu
from jax.sharding import PartitionSpec as P

momentum_decay = 0.9
square_decay = 0.95
adam_epsilon = 1e-08
update_scale = 0.25
learning_rate = 0.01

MESH = pl.DeviceIdType.MESH
CORES = 2
LANES = 128
f32 = jnp.float32
bf16 = jnp.bfloat16


def digits(fs, tp):
    xs = tp // CORES
    ys = xs if fs % xs == 0 else 1
    return fs // ys, ys, xs


def moments(scaled, first, second):
    return (momentum_decay * first + (1.0 - momentum_decay) * scaled,
            square_decay * second + (1.0 - square_decay) * scaled * scaled)


def exchange_kernel(
    fs, tp,
    x_v, c_v, x_o, c_o, fac_v, fac_o, w_v, w_o, m1_v, m2_v, m1_o, m2_o,
    F, W_v, W_o, R, S,
    xv, cv, xo, co, hi, rest,
    wown_v, wown_o,
    cs_v, cr_v, cs_o, cr_o, keep_v, keep_o,
    xs_v, xr_v, xs_o, xr_o, acc_v, acc_o,
    ys_v, yr_v, ys_o, yr_o, mid_v, mid_o,
    zs_v, zr_v, zs_o, zr_o, sq_s, sq_r,
    load_sem, fa_s, fa_r, fb_s, fb_r, fc_s, fc_r,
    wl_sem, wz_s, wz_r, wy_s, wy_r,
    rc_s, rc_r, rx_s, rx_r, ry_s, ry_r, rz_s, rz_r, sq_ss, sq_rs, ra_s, ra_r,
):
    Z, Y, X = digits(fs, tp)
    n = fs * tp
    f = lax.axis_index("fs")
    t = lax.axis_index("tp")
    z, y = f // Y, f % Y
    x, c = t // CORES, t % CORES
    me = f * tp + t

    def remote(src, dst, ss, rs, fd, td):
        return pltpu.make_async_remote_copy(
            src_ref=src, dst_ref=dst, send_sem=ss, recv_sem=rs,
            device_id={"fs": fd, "tp": td}, device_id_type=MESH)

    loads = [
        pltpu.make_async_copy(a, b, load_sem.at[i])
        for i, (a, b) in enumerate(((x_o, xo), (c_o, co), (x_v, xv), (c_v, cv)))
    ]
    for cp in loads:
        cp.start()

    barrier = pltpu.get_barrier_semaphore()

    @pl.loop(1, n)
    def _(d):
        peer = lax.rem(me + d, n)
        pl.semaphore_signal(
            barrier, inc=1, device_id={"fs": peer // tp, "tp": lax.rem(peer, tp)},
            device_id_type=MESH)

    rv, ro = fac_v.shape[0], fac_o.shape[0]
    F[pl.ds(f, 1), :rv, :] = fac_v[...][None]
    F[pl.ds(f, 1), rv:, :] = fac_o[...][None]
    wown_v[...] = w_v[...].astype(bf16)
    wown_o[...] = w_o[...].astype(bf16)
    pl.semaphore_wait(barrier, n - 1)

    rx = (rv + ro) // X

    def piece(fi, xi, ci):
        return F.at[fi, pl.ds(pl.multiple_of(xi * rx, 16), rx),
                    pl.ds(pl.multiple_of(ci * LANES, LANES), LANES)]

    def half(fi, ci):
        return F.at[fi, :, pl.ds(pl.multiple_of(ci * LANES, LANES), LANES)]

    def fa(d, fi):
        return remote(piece(fi, x, c), piece(fi, x, c), fa_s.at[d - 1], fa_r.at[d - 1],
                      lax.rem(f + d, fs), t)

    for d in range(1, fs):
        fa(d, f).start()

    parts = ((0, wown_v, W_v), (1, wown_o, W_o))
    own_copies = [pltpu.make_async_copy(own, W.at[z, y], wl_sem.at[p]) for p, own, W in parts]
    for cp in own_copies:
        cp.start()

    def wz(p, W, s, up, zb, src=None):
        k = 0 if up else 1
        zd = z + 1 if up else z - 1
        return remote(W.at[zb, y] if src is None else src, W.at[zb, y],
                      wz_s.at[p, k, s], wz_r.at[p, k, s], zd * Y + y, t)

    def wy(p, W, zb, d, yb, src=None):
        return remote(W.at[zb, yb] if src is None else src, W.at[zb, yb],
                      wy_s.at[p, zb, d - 1], wy_r.at[p, zb, d - 1],
                      z * Y + lax.rem(y + d, Y), t)

    def weights_send(s):
        @pl.when((z >= s) & (z < Z - 1))
        def _():
            for p, own, W in parts:
                wz(p, W, s, True, z - s, own if s == 0 else None).start()

        @pl.when((z + s < Z) & (z > 0))
        def _():
            for p, own, W in parts:
                wz(p, W, s, False, z + s, own if s == 0 else None).start()

    def weights_receive(s):
        for up in (True, False):
            zb = z - 1 - s if up else z + 1 + s

            @pl.when((zb >= 0) if up else (zb < Z))
            def _():
                for p, own, W in parts:
                    wz(p, W, s, up, zb).wait_recv()
                    for d in range(1, Y):
                        wy(p, W, zb, d, y).start()

    weights_send(0)
    for p, own, W in parts:
        for d in range(1, Y):
            wy(p, W, z, d, y, own).start()

    def fb(d, k, fi, xi):
        return remote(piece(fi, xi, c), piece(fi, xi, c), fb_s.at[d - 1, k - 1],
                      fb_r.at[d - 1, k - 1], f, lax.rem(x + k, X) * CORES + c)

    def fc(d, fi, ci):
        return remote(half(fi, ci), half(fi, ci), fc_s.at[d - 1], fc_r.at[d - 1],
                      f, x * CORES + 1 - c)

    source = [lax.rem(f + fs - d, fs) for d in range(fs)]
    for d in range(1, fs):
        fa(d, source[d]).wait_recv()
        for k in range(1, X):
            fb(d, k, source[d], x).start()
    for d in range(1, fs):
        for k in range(1, X):
            fb(d, k, source[d], lax.rem(x + X - k, X)).wait_recv()
        fc(d, source[d], c).start()
    for d in range(1, fs):
        fc(d, source[d], 1 - c).wait_recv()

    tokens = xo.shape[0]
    step = tokens // 4

    def basis(x_ref, rows):
        @pl.loop(0, tokens // step)
        def _(i):
            at = pl.ds(pl.multiple_of(i * step, step), step)
            fac = F[:, rows, :].reshape(-1, F.shape[2])
            b = jnp.dot(x_ref[at, :], fac, preferred_element_type=f32).T
            high = b.astype(bf16)
            hi[:, at] = high
            rest[:, at] = (b - high.astype(f32)).astype(bf16)

    def product(c_ref, start, width):
        cols = c_ref[:, pl.ds(pl.multiple_of(start, LANES), width)]
        return (jnp.dot(hi[...], cols, preferred_element_type=f32)
                + jnp.dot(rest[...], cols, preferred_element_type=f32))

    def rc(p, send, recv, i):
        return remote(send.at[i], recv.at[i], rc_s.at[p, i], rc_r.at[p, i],
                      f, x * CORES + 1 - c)

    def multiply(p, c_ref, send, recv, keep):
        cb = keep.shape[2]

        @pl.loop(0, X)
        def _(i):
            send[i] = product(c_ref, (i * CORES + 1 - c) * cb, cb)
            rc(p, send, recv, i).start()

        @pl.loop(0, X)
        def _(i):
            keep[i] = product(c_ref, (i * CORES + c) * cb, cb)

    def sx(p, send, recv, k):
        xd = lax.rem(x + k, X)
        return remote(send.at[k - 1], recv.at[k - 1], rx_s.at[p, k - 1], rx_r.at[p, k - 1],
                      f, xd * CORES + c)

    def sy(p, send, recv, k):
        yd = lax.rem(y + k, Y)
        return remote(send.at[k - 1], recv.at[k - 1], ry_s.at[p, k - 1], ry_r.at[p, k - 1],
                      z * Y + yd, t)

    def sz(p, send, recv, k):
        zd = lax.rem(z + k, Z)
        return remote(send.at[k - 1], recv.at[k - 1], rz_s.at[p, k - 1], rz_r.at[p, k - 1],
                      zd * Y + y, t)

    def to_x(p, cs, cr, keep, send, recv):
        for i in range(X):
            rc(p, cs, cr, i).wait_recv()
        for k in range(1, X):
            xd = lax.rem(x + k, X)
            send[k - 1] = (keep[xd] + cr[xd]).astype(bf16)
            sx(p, send, recv, k).start()

    def to_y(p, cr, keep, xsend, recv, acc, send, yrecv):
        total = keep[x] + cr[x]
        for k in range(1, X):
            sx(p, xsend, recv, k).wait_recv()
            total = total + recv[k - 1].astype(f32)
        acc[...] = total.reshape(acc.shape)
        for k in range(1, Y):
            yd = lax.rem(y + k, Y)
            send[k - 1] = acc[:, pl.ds(yd, 1)][:, 0].astype(bf16)
            sy(p, send, yrecv, k).start()

    def to_z(p, acc, ysend, recv, mid, send, zrecv):
        total = acc[:, pl.ds(y, 1)][:, 0]
        for k in range(1, Y):
            sy(p, ysend, recv, k).wait_recv()
            total = total + recv[k - 1].astype(f32)
        mid[...] = total
        for k in range(1, Z):
            send[k - 1] = mid[lax.rem(z + k, Z)].astype(bf16)
            sz(p, send, zrecv, k).start()

    def finish(p, mid, send, recv):
        total = mid[z]
        for k in range(1, Z):
            sz(p, send, recv, k).wait_recv()
            total = total + recv[k - 1].astype(f32)
        return total

    loads[0].wait()
    basis(xo, slice(rv, rv + ro))
    loads[1].wait()
    multiply(1, co, cs_o, cr_o, keep_o)
    to_x(1, cs_o, cr_o, keep_o, xs_o, xr_o)
    if Z > 1:
        weights_receive(0)
    if Z > 2:
        weights_send(1)
    loads[2].wait()
    basis(xv, slice(0, rv))
    loads[3].wait()
    multiply(0, cv, cs_v, cr_v, keep_v)
    to_x(0, cs_v, cr_v, keep_v, xs_v, xr_v)
    to_y(1, cr_o, keep_o, xs_o, xr_o, acc_o, ys_o, yr_o)
    to_y(0, cr_v, keep_v, xs_v, xr_v, acc_v, ys_v, yr_v)
    to_z(1, acc_o, ys_o, yr_o, mid_o, zs_o, zr_o)
    to_z(0, acc_v, ys_v, yr_v, mid_v, zs_v, zr_v)
    for s in range(1, Z - 1):
        weights_receive(s)
        if s + 1 < Z - 1:
            weights_send(s + 1)
    low_o = finish(1, mid_o, zs_o, zr_o)
    low_v = finish(0, mid_v, zs_v, zr_v)

    square = jnp.sum(low_o * low_o) + jnp.sum(low_v * low_v)
    sq_s[...] = jnp.full(sq_s.shape, square, f32)

    @pl.loop(1, n)
    def _(d):
        peer = lax.rem(me + d, n)
        remote(sq_s, sq_r.at[d - 1], sq_ss.at[d - 1], sq_rs.at[d - 1],
               peer // tp, lax.rem(peer, tp)).start()

    @pl.loop(1, n)
    def _(d):
        remote(sq_s, sq_r.at[d - 1], sq_ss.at[d - 1], sq_rs.at[d - 1], f, t).wait_recv()

    total = jnp.sum(sq_r[...], axis=0)[0:1, 0:1] + square
    count = hi.shape[0] * (cv.shape[1] + co.shape[1])
    clip = 1.0 / jnp.maximum(jnp.sqrt(total / count), 1.0)

    cbv = low_v.shape[1]
    for cols, low, m1, m2 in (
        (slice(0, cbv), low_v, m1_v, m2_v), (slice(cbv, None), low_o, m1_o, m2_o)
    ):
        scaled = clip * low
        S[:, cols] = scaled
        first, second = moments(scaled, m1[...], m2[...])
        R[pl.ds(f, 1), :, cols] = (first / (jnp.sqrt(second) + adam_epsilon)).astype(bf16)[None]

    def ra(d, fi):
        return remote(R.at[fi], R.at[fi], ra_s.at[d - 1], ra_r.at[d - 1], lax.rem(f + d, fs), t)

    for d in range(1, fs):
        ra(d, f).start()

    for cp in own_copies:
        cp.wait()
    for s in range(Z - 1):
        @pl.when((z >= s) & (z < Z - 1))
        def _():
            for p, own, W in parts:
                wz(p, W, s, True, z - s, own if s == 0 else None).wait_send()

        @pl.when((z + s < Z) & (z > 0))
        def _():
            for p, own, W in parts:
                wz(p, W, s, False, z + s, own if s == 0 else None).wait_send()
    for p, own, W in parts:
        for zb in range(Z):
            for d in range(1, Y):
                wy(p, W, zb, d, y).wait_send()
                wy(p, W, zb, d, lax.rem(y + Y - d, Y)).wait_recv()
    for d in range(1, fs):
        fa(d, f).wait_send()
        for k in range(1, X):
            fb(d, k, source[d], x).wait_send()
        fc(d, source[d], c).wait_send()
    for p, cs, cr, xsnd, xrcv, ysnd, yrcv, zsnd, zrcv in (
        (0, cs_v, cr_v, xs_v, xr_v, ys_v, yr_v, zs_v, zr_v),
        (1, cs_o, cr_o, xs_o, xr_o, ys_o, yr_o, zs_o, zr_o),
    ):
        for i in range(X):
            rc(p, cs, cr, i).wait_send()
        for k in range(1, X):
            sx(p, xsnd, xrcv, k).wait_send()
        for k in range(1, Y):
            sy(p, ysnd, yrcv, k).wait_send()
        for k in range(1, Z):
            sz(p, zsnd, zrcv, k).wait_send()

    @pl.loop(1, n)
    def _(d):
        remote(sq_s, sq_r.at[d - 1], sq_ss.at[d - 1], sq_rs.at[d - 1], f, t).wait_send()

    for d in range(1, fs):
        ra(d, f).wait_send()
        ra(d, source[d]).wait_recv()


def update_kernel(
    F, W_v, W_o, R, S, w_v, w_o, m1_v, m2_v, m1_o, m2_o,
    u_v, u_o, nw_v, nw_o, copy_v, copy_o, n1_v, n2_v, n1_o, n2_o,
):
    f = lax.axis_index("fs")
    step = pl.program_id(0)
    group = F.shape[0]
    rv, ro = w_v.shape[0], w_o.shape[0]
    cbv = w_v.shape[1]
    rank = F.shape[2]
    rate = learning_rate * update_scale

    parts = (
        (slice(0, rv), slice(0, cbv), W_v, w_v, u_v, nw_v, copy_v),
        (slice(rv, rv + ro), slice(cbv, None), W_o, w_o, u_o, nw_o, copy_o),
    )
    for rows, cols, W, w, u, nw, copy in parts:
        fac = F[:, rows, :].reshape(-1, rank)
        ratio = R[...].reshape(rank, -1)[:, cols]
        change = jnp.dot(fac, ratio, preferred_element_type=f32)
        copy[...] = (W[...].astype(f32).reshape(change.shape) - rate * change).astype(bf16)

    @pl.when(step == f // group)
    def _():
        for rows, cols, W, w, u, nw, copy in parts:
            ratio = R[...].reshape(rank, -1)[:, cols]
            mine = jnp.dot(F[pl.ds(f % group, 1), rows, :][0], ratio, preferred_element_type=f32)
            update = update_scale * mine
            u[...] = update
            nw[...] = w[...] - learning_rate * update

    @pl.when(step == 0)
    def _():
        n1_v[...], n2_v[...] = moments(S[:, :cbv], m1_v[...], m2_v[...])
        n1_o[...], n2_o[...] = moments(S[:, cbv:], m1_o[...], m2_o[...])


def solution(mesh):
    fs, tp = mesh.shape["fs"], mesh.shape["tp"]
    Z, Y, X = digits(fs, tp)

    def shards(x_v, c_v, x_o, c_o, fac_v, fac_o, w_v, w_o, m1_v, m2_v, m1_o, m2_o):
        rank = fac_v.shape[1]
        rr = rank // fs
        cbv, cbo = w_v.shape[1], w_o.shape[1]
        tokens = x_v.shape[0]
        vmem = pl.BlockSpec(memory_space=pltpu.VMEM)
        hbm = pl.BlockSpec(memory_space=pl.ANY)
        sds = jax.ShapeDtypeStruct
        V = pltpu.VMEM
        dma = pltpu.SemaphoreType.DMA

        def both(shape_of, dtype, copies=2):
            out = []
            for cb in (cbv, cbo):
                out += [V(shape_of(cb), dtype)] * copies
            return out

        x1, y1, z1 = max(X - 1, 1), max(Y - 1, 1), max(Z - 1, 1)
        scratch = [
            V(x_v.shape, bf16), V(c_v.shape, bf16), V(x_o.shape, bf16), V(c_o.shape, bf16),
            V((rank, tokens), bf16), V((rank, tokens), bf16),
            V(w_v.shape, bf16), V(w_o.shape, bf16),
            *both(lambda cb: (X, rank, cb), f32), *both(lambda cb: (X, rank, cb), f32, 1),
            *both(lambda cb: (x1, rank, cb), bf16),
            *both(lambda cb: (Z, Y, rr, cb), f32, 1),
            *both(lambda cb: (y1, Z, rr, cb), bf16),
            *both(lambda cb: (Z, rr, cb), f32, 1),
            *both(lambda cb: (z1, rr, cb), bf16),
            V((1, LANES), f32), V((fs * tp - 1, 1, LANES), f32),
            dma((4,)), dma((fs - 1,)), dma((fs - 1,)), dma((fs - 1, x1)), dma((fs - 1, x1)),
            dma((fs - 1,)), dma((fs - 1,)),
            dma((2,)), dma((2, 2, z1)), dma((2, 2, z1)), dma((2, Z, y1)), dma((2, Z, y1)),
            dma((2, X)), dma((2, X)), dma((2, x1)), dma((2, x1)), dma((2, y1)), dma((2, y1)),
            dma((2, z1)), dma((2, z1)), dma((fs * tp - 1,)), dma((fs * tp - 1,)),
            dma((fs - 1,)), dma((fs - 1,)),
        ]
        rows = fac_v.shape[0] + fac_o.shape[0]
        F, W_v, W_o, R, S = pl.pallas_call(
            functools.partial(exchange_kernel, fs, tp),
            out_shape=(
                sds((fs, rows, rank), bf16), sds((Z, Y) + w_v.shape, bf16),
                sds((Z, Y) + w_o.shape, bf16), sds((fs, rr, cbv + cbo), bf16),
                sds((rr, cbv + cbo), f32),
            ),
            in_specs=[hbm] * 4 + [vmem] * 8,
            out_specs=(vmem, hbm, hbm, vmem, vmem),
            scratch_shapes=scratch,
            compiler_params=pltpu.CompilerParams(
                collective_id=0, has_side_effects=True, vmem_limit_bytes=60 * 1024 * 1024),
            name="exchange",
        )(x_v, c_v, x_o, c_o, fac_v, fac_o, w_v, w_o, m1_v, m2_v, m1_o, m2_o)
        group = Y

        def whole(a):
            return pl.BlockSpec(a.shape, lambda i: (0,) * len(a.shape))

        def tall(a):
            return pl.BlockSpec((group * a.shape[0], a.shape[1]), lambda i: (i, 0))

        def stack(a):
            return pl.BlockSpec((1, group) + a.shape, lambda i: (i, 0, 0, 0))

        small = (m1_v, m2_v, m1_o, m2_o)
        return pl.pallas_call(
            update_kernel,
            grid=(fs // group,),
            out_shape=(
                sds(w_v.shape, f32), sds(w_o.shape, f32),
                sds(w_v.shape, f32), sds(w_o.shape, f32),
                sds((fs * w_v.shape[0], cbv), bf16), sds((fs * w_o.shape[0], cbo), bf16),
                *[sds(a.shape, f32) for a in small],
            ),
            in_specs=[
                pl.BlockSpec((group, rows, rank), lambda i: (i, 0, 0)), stack(w_v), stack(w_o),
                whole(R), whole(S), whole(w_v), whole(w_o), *[whole(a) for a in small],
            ],
            out_specs=(
                whole(w_v), whole(w_o), whole(w_v), whole(w_o), tall(w_v), tall(w_o),
                *[whole(a) for a in small],
            ),
            compiler_params=pltpu.CompilerParams(vmem_limit_bytes=60 * 1024 * 1024),
            name="update",
        )(F, W_v, W_o, R, S, w_v, w_o, *small)

    fsp = P(("fs", "tp"), None)
    both = P("fs", "tp")
    return jax.shard_map(
        shards,
        mesh=mesh,
        in_specs=(fsp,) * 4 + (P("fs", None),) * 2 + (both,) * 6,
        out_specs=(both,) * 4 + (P(None, "tp"),) * 2 + (both,) * 4,
        check_vma=False,
    )
```
